32 devices in a mesh: ep: 8 (over z, x), tp: 4 (over y, core).
Axes of the slice: x: 2, y: 2, z: 4, core: 2. Of those that a mesh axis runs over, the one named last changes fastest.
Arguments:
- memory_query_matrix: bfloat16 [4096, 1024], P('ep', 'tp'), may hold values from -0.59765625 to 2
- memory_key_matrix: bfloat16 [4096, 1024], P('ep', 'tp'), may hold values from -0.59765625 to 2
- memory_value_matrix: bfloat16 [4096, 1024], P('ep', 'tp'), may hold values from -6 to 6
- input_gate_logits: float32 [4, 4096], P('tp', 'ep'), may hold values from -6 to 260
- forget_gate_logits: float32 [4, 4096], P('tp', 'ep'), may hold values from -1 to 20
- forget_log_boosts: float32 [4, 4096], P('tp', 'ep'), may hold values from -0.7 to 0
- head_norm_scale: float32 [1024], P('tp'), may hold values from 0.1 to 1.9
- memory_output_matrix: bfloat16 [1024, 2048], replicated, may hold values from -0.1875 to 0.1875
- projection_norm_scale: float32 [2048], replicated, may hold values from 0.1 to 1.9
- second_batch_rows: bfloat16 [6144, 2048], P(('ep', 'tp')), may hold values from -6 to 6
- expert_prenorm_scale: float32 [2048], replicated, may hold values from 0.1 to 1.9
- selected_expert_index: int32 [6144, 2], P(('ep', 'tp')), may hold values from 0 to 7, all different within a row; in each aligned block of 192 rows (0 to 191, 192 to 383, ...) at most 96 rows name the same one
- group_route_probability: float32 [6144], P(('ep', 'tp')), may hold values from 0.2 to 1
- expert_choice_scores: float32 [6144, 2], P(('ep', 'tp')), may hold values from -6 to 6
- expert_gate_matrix: bfloat16 [8, 2048, 512], P('ep'), may hold values from -0.125 to 0.125
- expert_up_matrix: bfloat16 [8, 2048, 512], P('ep'), may hold values from -0.125 to 0.125
- expert_down_matrix: bfloat16 [8, 512, 2048], P('ep'), may hold values from -0.25 to 0.25
Outputs:
- mixed_rows: bfloat16 [4096, 2048], P(('ep', 'tp'))
- routed_rows: bfloat16 [6144, 2048], P(('ep', 'tp'))
The draws below stay inside these ranges and needn't reach their ends.
Inputs may be any that keep to these rules, and one draw needn't show every extreme that they name: `selected_expert_index`: each row names 2 different experts; among the rows of one device no expert is named more than 96 times, and in some device one expert is named exactly that often.
All inputs are finite; a program needn't handle non-finite values.
Results may differ from the reference program's by a relative error of at most 0.013.
Values may be sent and summed in bfloat16 or wider, within the bound.
A program may use at most 128 MiB of HBM per device.

```python
import math
import jax
import jax.numpy as jnp
import numpy as np
from jax import lax

D = 2048
HEADS = 4
HEAD_SIZE = 256
CELL_WIDTH = 1024
SPAN = 128
MIX_DEV = 512
SEQ_LEN = 4096
EXPERT_HIDDEN = 512
TOPK = 2
ROUTED_DEV = 192
ROUTED = 6144
EXPERTS = 8
CAPACITY = 96


def draw_forget_gate_logits(key, part):
    keys = jax.random.split(jax.random.fold_in(key, 71), 3)
    order = jax.random.permutation(keys[0], HEADS)
    quick = HEADS // 2
    slow_bias = math.log(SEQ_LEN) + 0.6
    bias = jnp.where(order < quick, 4.2, slow_bias).astype(jnp.float32)
    pieces = SEQ_LEN // MIX_DEV
    offset = jax.random.uniform(keys[1], (HEADS, pieces, 1), jnp.float32, -0.7, 0.7)
    offset = jnp.broadcast_to(offset, (HEADS, pieces, MIX_DEV)).reshape(HEADS, SEQ_LEN)
    noise = jnp.clip(jax.random.normal(keys[2], (HEADS, SEQ_LEN), jnp.float32), -4.0, 4.0)
    return bias[:, None] + offset + noise


def draw_forget_log_boosts(key, part):
    keys = jax.random.split(jax.random.fold_in(key, 83), 2)
    spots = jax.random.randint(keys[0], (HEADS, 3), 0, SEQ_LEN)
    depth = jax.random.uniform(keys[1], (HEADS, 3), jnp.float32, -0.69, -0.22)
    places = jnp.arange(SEQ_LEN, dtype=jnp.int32)
    hits = places[None, None, :] == spots[:, :, None]
    return jnp.min(jnp.where(hits, depth[:, :, None], 0.0), axis=1)


def draw_input_gate_logits(key, part):
    keys = jax.random.split(jax.random.fold_in(key, 97), 1)
    return jnp.clip(jax.random.normal(keys[0], (HEADS, SEQ_LEN), jnp.float32), -6.0, 6.0)


def shard_levels(stream_key, dims, shards, least, high):
    def one(dim, shards_of):
        heights = jax.random.uniform(jax.random.fold_in(jax.random.fold_in(stream_key, 6), dim), (shards_of,), jnp.float32, least / len(shards), high / len(shards))
        return jnp.repeat(jnp.exp(heights), dims[dim] // shards_of).reshape((-1,) + (1,) * (len(dims) - dim - 1))

    loudness = one(*shards[0])
    for cut in shards[1:]:
        loudness = loudness * one(*cut)
    return loudness


def shared_out(own_key, own, number, rows, count, top, most, skew):
    order = jax.random.permutation(own_key, count)
    packed, ordinary = portions_of(count, rows * top, most, skew, True), portions_of(count, rows * top, most, skew, False)
    places = jnp.arange(count)

    def named(sizes, turn):
        used = int((sizes > 0).sum())
        fixed = max(1, used // 4)
        passed = fixed + (places - fixed + turn * (used - fixed)) % max(1, count - fixed)
        return jnp.zeros((count,), jnp.int32).at[order[jnp.where(places < fixed, places, passed)]].set(jnp.asarray(sizes, jnp.int32))

    sizes = jnp.where(number % 4 == 0, named(packed, number // 4), named(ordinary, number - number // 4 - 1))
    mixed = jax.random.permutation(jax.random.fold_in(own, 3), count)
    giver, sink = mixed[0:count // 2 * 2:2], mixed[1:count // 2 * 2:2]
    slack = jnp.minimum(sizes[giver] - 1, most - sizes[sink]) // 2
    slack = jnp.where((giver == order[0]) | (sink == order[0]) | (sizes[sink] == 0), 0, jnp.maximum(slack, 0))
    passed = jax.random.randint(jax.random.fold_in(own, 4), (count // 2,), 0, 1 << 20) % (slack + 1)
    sizes = sizes.at[giver].add(-passed).at[sink].add(passed)
    items = jnp.searchsorted(jnp.cumsum(sizes), jnp.arange(rows * top), side="right").astype(jnp.int32)
    table = items.reshape(top, rows).T
    table = table[jax.random.permutation(jax.random.fold_in(own, 1), rows)]
    turn = jax.random.randint(jax.random.fold_in(own, 2), (rows, 1), 0, top)
    return jnp.take_along_axis(table, (jnp.arange(top)[None, :] + turn) % top, axis=1)


def portions_of(count, total, most, lean, full):
    portions = [(1 << 20) // math.isqrt(standing ** lean) + 1 for standing in range(1, count + 1)]
    largest = most if full else min(most, max(-(-total // count), total * portions[0] // sum(portions)))
    least = 1 if total - largest >= count - 1 else 0
    given, surplus = [largest] + [least] * (count - 1), total - largest - least * (count - 1)
    while surplus > 0:
        free = [i for i in range(1, count) if given[i] < largest] or [i for i in range(1, count) if given[i] < most]
        mass, left = sum([portions[i] for i in free]), surplus
        for i in free:
            extra = min(most - given[i], max(1, left * portions[i] // mass), surplus)
            given[i] = given[i] + extra
            surplus = surplus - extra
    return np.array(given)


def bell_draw(own_key, dims, deviation, limit, cuts=(), held_as=jnp.bfloat16):
    array = deviation * jax.random.normal(own_key, dims, jnp.float32)
    if cuts:
        array = array * shard_levels(own_key, dims, cuts, -0.22, 0.18)
    return jnp.clip(array, -limit, limit).astype(held_as)


def setup_inputs(seed: int = 0) -> dict:
    key_of = jax.random.split(jax.random.key(seed), 18)
    memory_query_matrix = jnp.clip(-0.59765625 + 2.5976562 * jax.random.uniform(key_of[0], (SEQ_LEN, CELL_WIDTH), jnp.float32) ** shard_levels(key_of[0], (SEQ_LEN, CELL_WIDTH), ((0, 8), (1, 4)), -0.2, 0.2), -0.59765625, 2.0).astype(jnp.bfloat16)
    memory_key_matrix = jnp.clip(-0.59765625 + 2.5976562 * jax.random.uniform(key_of[1], (SEQ_LEN, CELL_WIDTH), jnp.float32) ** shard_levels(key_of[1], (SEQ_LEN, CELL_WIDTH), ((0, 8), (1, 4)), -0.2, 0.2), -0.59765625, 2.0).astype(jnp.bfloat16)
    memory_value_matrix = bell_draw(key_of[2], (SEQ_LEN, CELL_WIDTH), 1.0, 6.0, ((0, 8), (1, 4)))
    input_gate_logits = draw_input_gate_logits(jax.random.fold_in(key_of[17], 71), 0)
    forget_gate_logits = draw_forget_gate_logits(jax.random.fold_in(key_of[17], 71), 0)
    forget_log_boosts = draw_forget_log_boosts(jax.random.fold_in(key_of[17], 71), 0)
    head_norm_scale = jnp.clip(1.0 + 0.18 * jax.random.normal(key_of[6], (CELL_WIDTH,), jnp.float32), 0.1, 1.9)
    memory_output_matrix = bell_draw(key_of[7], (CELL_WIDTH, D), CELL_WIDTH ** -0.5, 0.1875)
    projection_norm_scale = jnp.clip(1.0 + 0.18 * jax.random.normal(key_of[8], (D,), jnp.float32), 0.1, 1.9)
    second_batch_rows = bell_draw(key_of[9], (ROUTED, D), 1.0, 6.0, ((0, 32),))
    expert_prenorm_scale = jnp.clip(1.0 + 0.18 * jax.random.normal(key_of[10], (D,), jnp.float32), 0.1, 1.9)
    selected_expert_index_keys = jax.random.split(jax.random.fold_in(key_of[11], 1), ROUTED // ROUTED_DEV)
    selected_expert_index_turns = jax.random.permutation(jax.random.fold_in(key_of[11], 3), ROUTED // ROUTED_DEV)
    selected_expert_index = jax.vmap(lambda own, number: shared_out(jax.random.fold_in(key_of[11], 2), own, number, ROUTED_DEV, EXPERTS, TOPK, CAPACITY, 1))(selected_expert_index_keys, selected_expert_index_turns).reshape((ROUTED, TOPK))
    group_route_probability = jnp.clip(0.2 + 0.8 * jax.random.uniform(key_of[12], (ROUTED,), jnp.float32) ** shard_levels(key_of[12], (ROUTED,), ((0, 32),), -0.2, 0.2), 0.2, 1.0)
    expert_choice_scores = bell_draw(key_of[13], (ROUTED, TOPK), 1.5, 6.0, ((0, 32),), jnp.float32)
    expert_gate_matrix = bell_draw(key_of[14], (EXPERTS, D, EXPERT_HIDDEN), D ** -0.5, 0.125, ((0, 8),))
    expert_up_matrix = bell_draw(key_of[15], (EXPERTS, D, EXPERT_HIDDEN), D ** -0.5, 0.125, ((0, 8),))
    expert_down_matrix = bell_draw(key_of[16], (EXPERTS, EXPERT_HIDDEN, D), EXPERT_HIDDEN ** -0.5, 0.25, ((0, 8),))
    return dict(memory_query_matrix=memory_query_matrix, memory_key_matrix=memory_key_matrix, memory_value_matrix=memory_value_matrix, input_gate_logits=input_gate_logits, forget_gate_logits=forget_gate_logits, forget_log_boosts=forget_log_boosts, head_norm_scale=head_norm_scale, memory_output_matrix=memory_output_matrix, projection_norm_scale=projection_norm_scale, second_batch_rows=second_batch_rows, expert_prenorm_scale=expert_prenorm_scale, selected_expert_index=selected_expert_index, group_route_probability=group_route_probability, expert_choice_scores=expert_choice_scores, expert_gate_matrix=expert_gate_matrix, expert_up_matrix=expert_up_matrix, expert_down_matrix=expert_down_matrix)


floor_log = -1e+30
norm_eps = 1e-06
exact = lax.Precision.HIGHEST

def rms_scale(values, gain):
    squares = lax.optimization_barrier(jnp.mean(values * values, axis=-1, keepdims=True))
    return values * lax.rsqrt(squares + norm_eps) * gain

def span_step(carry, inputs):
    memory, normer, stabil = carry
    query, keyrow, valrow, in_gate, log_retain_factor = inputs
    key_scale = query.shape[-1] ** (-0.5)
    length = query.shape[1]
    causal = jnp.tril(jnp.ones((length, length), dtype=bool))
    cumulative = jnp.cumsum(log_retain_factor, axis=-1)
    decay_map = cumulative[:, :, None] - cumulative[:, None, :] + in_gate[:, None, :]
    decay_map = jnp.where(causal[None], decay_map, -jnp.inf)
    carried = cumulative + stabil[:, None]
    peak = jnp.maximum(carried, lax.optimization_barrier(jnp.max(decay_map, axis=-1)))
    within = jnp.exp(decay_map - peak[:, :, None])
    across = jnp.exp(carried - peak)
    qfloat = query.astype(jnp.float32)
    products = jnp.einsum('htd,hsd->hts', qfloat, keyrow.astype(jnp.float32))
    scores = products * key_scale * within
    denominator = lax.optimization_barrier(jnp.sum(scores, axis=-1)) + across * jnp.einsum('hd,htd->ht', normer, qfloat, precision=exact)
    weights = scores.astype(jnp.bfloat16)
    numerator = jnp.einsum('hts,hsd->htd', weights.astype(jnp.float32), valrow.astype(jnp.float32))
    numerator = numerator + across[:, :, None] * jnp.einsum('hed,htd->hte', memory, qfloat, precision=exact)
    output = numerator / jnp.maximum(jnp.abs(denominator), jnp.exp(-peak))[:, :, None]
    span_end = cumulative[:, -1]
    gap_log = span_end[:, None] - cumulative + in_gate
    new_peak = jnp.maximum(span_end + stabil, lax.optimization_barrier(jnp.max(gap_log, axis=-1)))
    shrink = jnp.exp(span_end + stabil - new_peak)
    spread = jnp.exp(gap_log - new_peak[:, None]) * key_scale
    keys_weighted = keyrow.astype(jnp.float32) * spread[:, :, None]
    memory = shrink[:, None, None] * memory + jnp.einsum('hse,hsd->hed', valrow.astype(jnp.float32), keys_weighted, precision=exact)
    normer = shrink[:, None] * normer + lax.optimization_barrier(jnp.sum(keys_weighted, axis=1))
    return ((memory, normer, new_peak), output)

def reference(memory_query_matrix, memory_key_matrix, memory_value_matrix, input_gate_logits, forget_gate_logits, forget_log_boosts, head_norm_scale, memory_output_matrix, projection_norm_scale, second_batch_rows, expert_prenorm_scale, selected_expert_index, group_route_probability, expert_choice_scores, expert_gate_matrix, expert_up_matrix, expert_down_matrix):
    spans = SEQ_LEN // SPAN

    def by_head(rows):
        return rows.reshape(SEQ_LEN, HEADS, HEAD_SIZE).transpose(1, 0, 2)

    def to_spans(values):
        shaped = values.reshape((HEADS, spans, SPAN) + values.shape[2:])
        return jnp.moveaxis(shaped, 1, 0)
    log_retain_factor = jax.nn.log_sigmoid(forget_gate_logits) + forget_log_boosts
    start = (jnp.zeros((HEADS, HEAD_SIZE, HEAD_SIZE), jnp.float32), jnp.zeros((HEADS, HEAD_SIZE), jnp.float32), jnp.full((HEADS,), floor_log, jnp.float32))
    inputs = (to_spans(by_head(memory_query_matrix)), to_spans(by_head(memory_key_matrix)), to_spans(by_head(memory_value_matrix)), to_spans(input_gate_logits), to_spans(log_retain_factor))
    _, cells = lax.scan(span_step, start, inputs)
    cells = jnp.moveaxis(cells, 0, 1).reshape(HEADS, SEQ_LEN, HEAD_SIZE)
    scaled = (cells * head_norm_scale.reshape(HEADS, 1, HEAD_SIZE)).astype(jnp.bfloat16)
    head_out = scaled.transpose(1, 0, 2).reshape(SEQ_LEN, CELL_WIDTH)
    projected = jnp.dot(head_out, memory_output_matrix, preferred_element_type=jnp.float32)
    mixed_rows = rms_scale(projected, projection_norm_scale).astype(jnp.bfloat16)
    ffn_rows = rms_scale(second_batch_rows.astype(jnp.float32), expert_prenorm_scale).astype(jnp.bfloat16)
    flat_ids = selected_expert_index.reshape(-1).astype(jnp.int32)
    owners = jnp.repeat(jnp.arange(ROUTED, dtype=jnp.int32), TOPK)
    onehot = (flat_ids[:, None] == jnp.arange(EXPERTS, dtype=jnp.int32)[None, :]).astype(jnp.int32)
    rank = lax.optimization_barrier(jnp.sum((jnp.cumsum(onehot, axis=0) - onehot) * onehot, axis=1)).astype(jnp.int32)
    slots = ROUTED // ROUTED_DEV * CAPACITY
    route_weight = group_route_probability[:, None] * jax.nn.softmax(expert_choice_scores, axis=-1)
    members = jnp.zeros((EXPERTS, slots), jnp.int32).at[flat_ids, rank].set(owners)
    shares = jnp.zeros((EXPERTS, slots), jnp.float32).at[flat_ids, rank].set(route_weight.reshape(-1))

    def one_expert(total, inputs):
        w_gate, w_up, w_down, member_rows, member_shares = inputs
        chosen = ffn_rows[member_rows]
        gate = jnp.dot(chosen, w_gate, preferred_element_type=jnp.float32)
        upper = jnp.dot(chosen, w_up, preferred_element_type=jnp.float32)
        hidden = (jax.nn.silu(gate) * upper).astype(jnp.bfloat16)
        answer = jnp.dot(hidden, w_down, preferred_element_type=jnp.float32).astype(jnp.bfloat16)
        total = total.at[member_rows].add(member_shares[:, None] * answer.astype(jnp.float32))
        return (total, None)
    total, _ = lax.scan(one_expert, jnp.zeros((ROUTED, D), jnp.float32), (expert_gate_matrix, expert_up_matrix, expert_down_matrix, members, shares))
    routed_rows = total.astype(jnp.bfloat16)
    return (mixed_rows, routed_rows)
```

```python
import functools

import jax
import jax.numpy as jnp
from jax import lax
from jax.experimental import pallas as pl
from jax.experimental.pallas import tpu as pltpu
from jax.sharding import PartitionSpec as P

FLOOR = -1e30
EPS = 1e-06
MESH = pl.DeviceIdType.MESH
F32 = jnp.float32
BF16 = jnp.bfloat16


def rms(values, gain):
    squares = jnp.mean(values * values, axis=-1, keepdims=True)
    return values * lax.rsqrt(squares + EPS) * gain


def dot(a, b, dims=((1,), (0,)), precision=None):
    return lax.dot_general(a, b, (dims, ((), ())), preferred_element_type=F32, precision=precision)


def join(early, late):
    total_e, peak_e, mem_e, nor_e = early
    total_l, peak_l, mem_l, nor_l = late
    peak = jnp.maximum(total_l + peak_e, peak_l)
    fe = jnp.exp(total_l + peak_e - peak)
    fl = jnp.exp(peak_l - peak)
    return (total_e + total_l, peak, fe * mem_e + fl * mem_l, fe * nor_e + fl * nor_l)


def kernel(
    n, nt, cap,
    q_ref, k_ref, v_ref, ig_ref, fg_ref, fb_ref, hs_ref, wo_hbm, ps_ref,
    x_ref, es_ref, ids_ref, grp_ref, sc_ref, wg_hbm, wu_hbm, wd_hbm,
    mixed_ref, routed_ref,
    wg, wu, wd, wo, out, recv, ans, back, ffn, acc,
    cpair, spair, cgrp, sgrp, ent, head, pout, prec,
    wsem, d_ss, d_rs, a_ss, a_rs, c1s, c1r, s1s, s1r, c2s, c2r, s2s, s2r, p_ss, p_rs,
):
    me = lax.axis_index("ep")
    tp = lax.axis_index("tp")
    groups = n // 2
    grp = me // 2
    par = lax.rem(me, 2)
    partner = me + 1 - 2 * par
    tokens, width = x_ref.shape
    length, hd = q_ref.shape
    rows = mixed_ref.shape[0]

    barrier = pltpu.get_barrier_semaphore()

    def greet(i, c):
        pl.semaphore_signal(barrier, inc=1, device_id=(lax.rem(me + i, n), tp), device_id_type=MESH)
        return c

    lax.fori_loop(1, n, greet, 0)
    for j in range(1, nt):
        pl.semaphore_signal(barrier, inc=1, device_id=(me, lax.rem(tp + j, nt)), device_id_type=MESH)

    loads = [
        pltpu.make_async_copy(wg_hbm.at[0], wg, wsem.at[0]),
        pltpu.make_async_copy(wu_hbm.at[0], wu, wsem.at[1]),
        pltpu.make_async_copy(wd_hbm.at[0], wd, wsem.at[2]),
        pltpu.make_async_copy(wo_hbm.at[pl.ds(pl.multiple_of(tp * hd, hd), hd)], wo, wsem.at[3]),
    ]
    for load in loads:
        load.start()

    fg = fg_ref[...]
    lk = jnp.minimum(fg, 0.0) - jnp.log1p(jnp.exp(-jnp.abs(fg))) + fb_ref[...]
    rid = lax.broadcasted_iota(jnp.int32, (length, length), 0)
    cid = lax.broadcasted_iota(jnp.int32, (length, length), 1)
    upper = (rid <= cid).astype(F32)
    b_row = dot(jnp.broadcast_to(lk, (8, length)), upper, precision=lax.Precision.HIGHEST)[0:1]
    i_row = ig_ref[...]
    last = b_row[:, length - 1 : length]
    g_row = last - b_row + i_row
    m_loc = jnp.max(g_row, axis=-1, keepdims=True)
    which = lax.broadcasted_iota(jnp.int32, (128, length), 0)
    cols = jnp.where(which == 0, b_row, g_row).T
    b_col = cols[:, 0:1]
    g_col = cols[:, 1:2]
    kw = k_ref[...].astype(F32) * (jnp.exp(g_col - m_loc) * (hd**-0.5))
    c_loc = dot(kw.astype(BF16), v_ref[...], ((0,), (0,)))
    n_loc = jnp.sum(kw, axis=0, keepdims=True)
    stat_id = lax.broadcasted_iota(jnp.int32, (8, hd), 0)

    def stats(total, peak, nor):
        return jnp.where(stat_id == 0, nor, jnp.where(stat_id == 1, peak, total))

    cpair[par] = c_loc.astype(BF16)
    spair[par] = stats(last, m_loc, n_loc)

    pl.semaphore_wait(barrier, n - 1 + nt - 1)

    def pair_copies():
        return [
            pltpu.make_async_remote_copy(
                src_ref=cpair.at[par], dst_ref=cpair.at[par], send_sem=c1s, recv_sem=c1r,
                device_id=(partner, tp), device_id_type=MESH),
            pltpu.make_async_remote_copy(
                src_ref=spair.at[par], dst_ref=spair.at[par], send_sem=s1s, recv_sem=s1r,
                device_id=(partner, tp), device_id_type=MESH),
        ]

    for copy in pair_copies():
        copy.start()

    ffn[...] = rms(x_ref[...].astype(F32), es_ref[...]).astype(BF16)
    ids = ids_ref[...]
    first, second = ids[:, 0:1], ids[:, 1:2]
    lane_e = lax.broadcasted_iota(jnp.int32, (tokens, n), 1)
    named = ((lane_e == first) | (lane_e == second)).astype(F32)
    tr = lax.broadcasted_iota(jnp.int32, (tokens, tokens), 0)
    tc = lax.broadcasted_iota(jnp.int32, (tokens, tokens), 1)
    rank = dot((tc < tr).astype(BF16), named.astype(BF16))
    slot_a = first * cap + jnp.sum(jnp.where(lane_e == first, rank, 0.0), axis=1, keepdims=True).astype(jnp.int32)
    slot_b = second * cap + jnp.sum(jnp.where(lane_e == second, rank, 0.0), axis=1, keepdims=True).astype(jnp.int32)
    score = sc_ref[...]
    ex = jnp.exp(score - jnp.max(score, axis=-1, keepdims=True))
    route = grp_ref[...] * (ex / jnp.sum(ex, axis=-1, keepdims=True))
    rw_a, rw_b = route[:, 0:1], route[:, 1:2]
    lane_c = lax.broadcasted_iota(jnp.int32, (tokens, cap), 1)

    def pack(e):
        lane = lane_c + e * cap
        place = ((lane == slot_a) | (lane == slot_b)).astype(BF16)
        out[e] = dot(place, ffn[...], ((0,), (0,))).astype(BF16)

    def offset(i):
        return n // 2 + jnp.where(lax.rem(i, 2) == 0, i // 2, -((i + 1) // 2))

    def dispatch_copy(e):
        return pltpu.make_async_remote_copy(
            src_ref=out.at[e], dst_ref=recv.at[me], send_sem=d_ss.at[e], recv_sem=d_rs.at[me],
            device_id=(e, tp), device_id_type=MESH)

    def dispatch_arrival(s):
        return pltpu.make_async_remote_copy(
            src_ref=out.at[s], dst_ref=recv.at[s], send_sem=d_ss.at[s], recv_sem=d_rs.at[s],
            device_id=(s, tp), device_id_type=MESH)

    def answer_copy(s):
        return pltpu.make_async_remote_copy(
            src_ref=ans.at[s], dst_ref=back.at[me], send_sem=a_ss.at[s], recv_sem=a_rs.at[me],
            device_id=(s, tp), device_id_type=MESH)

    def answer_arrival(e):
        return pltpu.make_async_remote_copy(
            src_ref=ans.at[e], dst_ref=back.at[e], send_sem=a_ss.at[e], recv_sem=a_rs.at[e],
            device_id=(e, tp), device_id_type=MESH)

    for copy in pair_copies():
        copy.wait_send()
    def pair_arrival():
        return [
            pltpu.make_async_remote_copy(
                src_ref=cpair.at[1 - par], dst_ref=cpair.at[1 - par], send_sem=c1s, recv_sem=c1r,
                device_id=(partner, tp), device_id_type=MESH),
            pltpu.make_async_remote_copy(
                src_ref=spair.at[1 - par], dst_ref=spair.at[1 - par], send_sem=s1s, recv_sem=s1r,
                device_id=(partner, tp), device_id_type=MESH),
        ]

    for copy in pair_arrival():
        copy.wait_recv()

    def unpack(c, s):
        return (s[2:3], s[1:2], c.astype(F32), s[0:1])

    both = join(unpack(cpair[0], spair[0]), unpack(cpair[1], spair[1]))
    cgrp[grp] = both[2].astype(BF16)
    sgrp[grp] = stats(both[0], both[1], both[3])

    def group_copies(g):
        to = (g * 2 + par, tp)
        return [
            pltpu.make_async_remote_copy(
                src_ref=cgrp.at[grp], dst_ref=cgrp.at[grp], send_sem=c2s.at[g], recv_sem=c2r.at[grp],
                device_id=to, device_id_type=MESH),
            pltpu.make_async_remote_copy(
                src_ref=sgrp.at[grp], dst_ref=sgrp.at[grp], send_sem=s2s.at[g], recv_sem=s2r.at[grp],
                device_id=to, device_id_type=MESH),
        ]

    def group_arrivals(g):
        at = (g * 2 + par, tp)
        return [
            pltpu.make_async_remote_copy(
                src_ref=cgrp.at[g], dst_ref=cgrp.at[g], send_sem=c2s.at[g], recv_sem=c2r.at[g],
                device_id=at, device_id_type=MESH),
            pltpu.make_async_remote_copy(
                src_ref=sgrp.at[g], dst_ref=sgrp.at[g], send_sem=s2s.at[g], recv_sem=s2r.at[g],
                device_id=at, device_id_type=MESH),
        ]

    def send_group(g, c):
        for copy in group_copies(g):
            copy.start()
        return c

    lax.fori_loop(grp + 1, groups, send_group, 0)

    def send_tokens(i, c):
        e = lax.rem(me + offset(i), n)
        pack(e)
        dispatch_copy(e).start()
        return c

    lax.fori_loop(0, n - 1, send_tokens, 0)
    pack(me)
    for load in loads:
        load.wait()

    def expert(chosen):
        gate = dot(chosen, wg[...])
        up = dot(chosen, wu[...])
        hidden = (gate / (1.0 + jnp.exp(-gate)) * up).astype(BF16)
        return dot(hidden, wd[...]).astype(BF16)

    ans[me] = expert(out[me])

    ent[...] = jnp.zeros(ent.shape, F32)
    row1 = jnp.zeros((1, hd), F32)

    def enter(g, carry):
        total, peak, nor = carry
        for copy in group_arrivals(g):
            copy.wait_recv()
        total, peak, mem, nor = join((total, peak, ent[...], nor), unpack(cgrp[g], sgrp[g]))
        ent[...] = mem
        return total, peak, nor

    total, peak, nor = lax.fori_loop(0, grp, enter, (row1, row1 + FLOOR, row1))
    joined = join((total, peak, ent[...], nor), unpack(cpair[0], spair[0]))
    odd = par == 1
    m_in = jnp.where(odd, joined[1], peak)
    n_in = jnp.where(odd, joined[3], nor)
    c_in = jnp.where(odd, joined[2], ent[...])

    carried = b_col + m_in[:, 0:1]
    decay = jnp.where(cid <= rid, b_col - b_row + i_row, -jnp.inf)
    peaks = jnp.maximum(carried, jnp.max(decay, axis=-1, keepdims=True))
    across = jnp.exp(carried - peaks)
    scores = dot(q_ref[...], k_ref[...], ((1,), (1,))) * (hd**-0.5) * jnp.exp(decay - peaks)
    qf = q_ref[...].astype(F32)
    den = jnp.sum(scores, axis=-1, keepdims=True) + across * jnp.sum(qf * n_in, axis=-1, keepdims=True)
    num = dot(scores.astype(BF16), v_ref[...]) + across * dot(q_ref[...], c_in.astype(BF16))
    cell = num / jnp.maximum(jnp.abs(den), jnp.exp(-peaks))
    head[...] = (cell * hs_ref[...]).astype(BF16)

    def part_copy(j):
        return pltpu.make_async_remote_copy(
            src_ref=pout.at[j], dst_ref=prec.at[tp], send_sem=p_ss.at[j], recv_sem=p_rs.at[tp],
            device_id=(me, j), device_id_type=MESH)

    def part_arrival(j):
        return pltpu.make_async_remote_copy(
            src_ref=pout.at[j], dst_ref=prec.at[j], send_sem=p_ss.at[j], recv_sem=p_rs.at[j],
            device_id=(me, j), device_id_type=MESH)

    def project(j):
        pout[j] = dot(head[pl.ds(pl.multiple_of(j * rows, rows), rows), :], wo[...]).astype(BF16)

    def send_part(i, c):
        j = lax.rem(tp + i, nt)
        project(j)
        part_copy(j).start()
        return c

    lax.fori_loop(1, nt, send_part, 0)
    project(tp)

    def serve(i, c):
        s = lax.rem(me - offset(i) + n, n)
        dispatch_arrival(s).wait_recv()
        ans[s] = expert(recv[s])
        answer_copy(s).start()
        return c

    lax.fori_loop(0, n - 1, serve, 0)

    def mix(i, total):
        j = lax.rem(tp + i, nt)
        part_arrival(j).wait_recv()
        return total + prec[j].astype(F32)

    projected = pout[tp].astype(F32)
    for i in range(1, nt):
        projected = mix(i, projected)
    mixed_ref[...] = rms(projected, ps_ref[...]).astype(BF16)

    def weigh(e, block):
        lane = lane_c + e * cap
        w = jnp.where(lane == slot_a, rw_a, jnp.where(lane == slot_b, rw_b, 0.0))
        high = w.astype(BF16)
        low = (w - high.astype(F32)).astype(BF16)
        return dot(high, block) + dot(low, block)

    acc[...] = weigh(me, ans[me])

    def collect(i, c):
        e = lax.rem(me + offset(i), n)
        answer_arrival(e).wait_recv()
        acc[...] += weigh(e, back[e])
        return c

    lax.fori_loop(0, n - 1, collect, 0)
    routed_ref[...] = acc[...].astype(BF16)

    def finish(i, c):
        e = lax.rem(me + i, n)
        dispatch_copy(e).wait_send()
        answer_copy(e).wait_send()
        return c

    lax.fori_loop(1, n, finish, 0)

    def finish_group(g, c):
        for copy in group_copies(g):
            copy.wait_send()
        return c

    lax.fori_loop(grp + 1, groups, finish_group, 0)
    for i in range(1, nt):
        part_copy(lax.rem(tp + i, nt)).wait_send()


def shards(
    n, nt,
    memory_query_matrix, memory_key_matrix, memory_value_matrix,
    input_gate_logits, forget_gate_logits, forget_log_boosts,
    head_norm_scale, memory_output_matrix, projection_norm_scale,
    second_batch_rows, expert_prenorm_scale, selected_expert_index,
    group_route_probability, expert_choice_scores,
    expert_gate_matrix, expert_up_matrix, expert_down_matrix,
):
    length, hd = memory_query_matrix.shape
    tokens, width = second_batch_rows.shape
    hidden = expert_gate_matrix.shape[2]
    cap = 2 * selected_expert_index.shape[1] * tokens // n
    cap = -(-cap // 16) * 16
    rows = length // nt
    vm = pl.BlockSpec(memory_space=pltpu.VMEM)
    hbm = pl.BlockSpec(memory_space=pl.ANY)
    dma = pltpu.SemaphoreType.DMA
    slots = pltpu.VMEM((n, cap, width), BF16)
    return pl.pallas_call(
        functools.partial(kernel, n, nt, cap),
        out_shape=(
            jax.ShapeDtypeStruct((rows, width), BF16),
            jax.ShapeDtypeStruct((tokens, width), BF16),
        ),
        in_specs=[vm] * 7 + [hbm] + [vm] * 6 + [hbm] * 3,
        out_specs=(vm, vm),
        scratch_shapes=[
            pltpu.VMEM((width, hidden), BF16),
            pltpu.VMEM((width, hidden), BF16),
            pltpu.VMEM((hidden, width), BF16),
            pltpu.VMEM((hd, width), BF16),
            slots, slots, slots, slots,
            pltpu.VMEM((tokens, width), BF16),
            pltpu.VMEM((tokens, width), F32),
            pltpu.VMEM((2, hd, hd), BF16),
            pltpu.VMEM((2, 8, hd), F32),
            pltpu.VMEM((n // 2, hd, hd), BF16),
            pltpu.VMEM((n // 2, 8, hd), F32),
            pltpu.VMEM((hd, hd), F32),
            pltpu.VMEM((length, hd), BF16),
            pltpu.VMEM((nt, rows, width), BF16),
            pltpu.VMEM((nt, rows, width), BF16),
            dma((4,)),
            dma((n,)), dma((n,)), dma((n,)), dma((n,)),
            dma, dma, dma, dma,
            dma((n // 2,)), dma((n // 2,)), dma((n // 2,)), dma((n // 2,)),
            dma((nt,)), dma((nt,)),
        ],
        compiler_params=pltpu.CompilerParams(
            collective_id=0, has_side_effects=True, vmem_limit_bytes=62 * 1024 * 1024
        ),
    )(
        memory_query_matrix, memory_key_matrix, memory_value_matrix,
        input_gate_logits, forget_gate_logits, forget_log_boosts,
        head_norm_scale[None], memory_output_matrix, projection_norm_scale[None],
        second_batch_rows, expert_prenorm_scale[None], selected_expert_index,
        group_route_probability[:, None], expert_choice_scores,
        expert_gate_matrix, expert_up_matrix, expert_down_matrix,
    )


def solution(mesh):
    return jax.shard_map(
        functools.partial(shards, mesh.shape["ep"], mesh.shape["tp"]),
        mesh=mesh,
        in_specs=(
            P("ep", "tp"), P("ep", "tp"), P("ep", "tp"),
            P("tp", "ep"), P("tp", "ep"), P("tp", "ep"),
            P("tp"), P(), P(),
            P(("ep", "tp"), None), P(), P(("ep", "tp"), None),
            P(("ep", "tp")), P(("ep", "tp"), None),
            P("ep", None, None), P("ep", None, None), P("ep", None, None),
        ),
        out_specs=(P(("ep", "tp"), None), P(("ep", "tp"), None)),
        check_vma=False,
    )
```

```python
import functools

import jax
import jax.numpy as jnp
from jax import lax
from jax.experimental import pallas as pl
from jax.experimental.pallas import tpu as pltpu
from jax.sharding import PartitionSpec as P

FLOOR = -1e30
EPS = 1e-06
MESH = pl.DeviceIdType.MESH
F32 = jnp.float32
BF16 = jnp.bfloat16


def rms(values, gain):
    squares = jnp.mean(values * values, axis=-1, keepdims=True)
    return values * lax.rsqrt(squares + EPS) * gain


def dot(a, b, dims=((1,), (0,)), precision=None):
    return lax.dot_general(a, b, (dims, ((), ())), preferred_element_type=F32, precision=precision)


def join(early, late):
    total_e, peak_e, mem_e, nor_e = early
    total_l, peak_l, mem_l, nor_l = late
    peak = jnp.maximum(total_l + peak_e, peak_l)
    fe = jnp.exp(total_l + peak_e - peak)
    fl = jnp.exp(peak_l - peak)
    return (total_e + total_l, peak, fe * mem_e + fl * mem_l, fe * nor_e + fl * nor_l)


def kernel(
    n, nt, cap,
    q_ref, k_ref, v_ref, ig_ref, fg_ref, fb_ref, hs_ref, wo_hbm, ps_ref,
    x_ref, es_ref, ids_ref, grp_ref, sc_ref, wg_hbm, wu_hbm, wd_hbm,
    mixed_ref, routed_ref,
    wg, wu, wd, wo, out, recv, ans, back, ffn, acc,
    cpair, spair, cgrp, sgrp, ent, head, pout, prec,
    wsem, d_ss, d_rs, a_ss, a_rs, c1s, c1r, s1s, s1r, c2s, c2r, s2s, s2r, p_ss, p_rs,
):
    me = lax.axis_index("ep")
    tp = lax.axis_index("tp")
    groups = n // 2
    grp = me // 2
    par = lax.rem(me, 2)
    partner = me + 1 - 2 * par
    tokens, width = x_ref.shape
    length, hd = q_ref.shape
    rows = mixed_ref.shape[0]

    barrier = pltpu.get_barrier_semaphore()

    def greet(i, c):
        pl.semaphore_signal(barrier, inc=1, device_id=(lax.rem(me + i, n), tp), device_id_type=MESH)
        return c

    lax.fori_loop(1, n, greet, 0)
    for j in range(1, nt):
        pl.semaphore_signal(barrier, inc=1, device_id=(me, lax.rem(tp + j, nt)), device_id_type=MESH)

    loads = [
        pltpu.make_async_copy(wg_hbm.at[0], wg, wsem.at[0]),
        pltpu.make_async_copy(wu_hbm.at[0], wu, wsem.at[1]),
        pltpu.make_async_copy(wd_hbm.at[0], wd, wsem.at[2]),
        pltpu.make_async_copy(wo_hbm.at[pl.ds(pl.multiple_of(tp * hd, hd), hd)], wo, wsem.at[3]),
    ]
    for load in loads:
        load.start()

    fg = fg_ref[...]
    lk = jnp.minimum(fg, 0.0) - jnp.log1p(jnp.exp(-jnp.abs(fg))) + fb_ref[...]
    rid = lax.broadcasted_iota(jnp.int32, (length, length), 0)
    cid = lax.broadcasted_iota(jnp.int32, (length, length), 1)
    upper = (rid <= cid).astype(F32)
    b_row = dot(jnp.broadcast_to(lk, (8, length)), upper, precision=lax.Precision.HIGHEST)[0:1]
    i_row = ig_ref[...]
    last = b_row[:, length - 1 : length]
    g_row = last - b_row + i_row
    m_loc = jnp.max(g_row, axis=-1, keepdims=True)
    which = lax.broadcasted_iota(jnp.int32, (128, length), 0)
    cols = jnp.where(which == 0, b_row, g_row).T
    b_col = cols[:, 0:1]
    g_col = cols[:, 1:2]
    kw = k_ref[...].astype(F32) * (jnp.exp(g_col - m_loc) * (hd**-0.5))
    c_loc = dot(kw.astype(BF16), v_ref[...], ((0,), (0,)))
    n_loc = jnp.sum(kw, axis=0, keepdims=True)
    stat_id = lax.broadcasted_iota(jnp.int32, (8, hd), 0)

    def stats(total, peak, nor):
        return jnp.where(stat_id == 0, nor, jnp.where(stat_id == 1, peak, total))

    cpair[par] = c_loc.astype(BF16)
    spair[par] = stats(last, m_loc, n_loc)

    pl.semaphore_wait(barrier, n - 1 + nt - 1)

    def pair_copies():
        return [
            pltpu.make_async_remote_copy(
                src_ref=cpair.at[par], dst_ref=cpair.at[par], send_sem=c1s, recv_sem=c1r,
                device_id=(partner, tp), device_id_type=MESH),
            pltpu.make_async_remote_copy(
                src_ref=spair.at[par], dst_ref=spair.at[par], send_sem=s1s, recv_sem=s1r,
                device_id=(partner, tp), device_id_type=MESH),
        ]

    for copy in pair_copies():
        copy.start()

    ffn[...] = rms(x_ref[...].astype(F32), es_ref[...]).astype(BF16)
    ids = ids_ref[...]
    first, second = ids[:, 0:1], ids[:, 1:2]
    lane_e = lax.broadcasted_iota(jnp.int32, (tokens, n), 1)
    named = ((lane_e == first) | (lane_e == second)).astype(F32)
    tr = lax.broadcasted_iota(jnp.int32, (tokens, tokens), 0)
    tc = lax.broadcasted_iota(jnp.int32, (tokens, tokens), 1)
    rank = dot((tc < tr).astype(BF16), named.astype(BF16))
    slot_a = first * cap + jnp.sum(jnp.where(lane_e == first, rank, 0.0), axis=1, keepdims=True).astype(jnp.int32)
    slot_b = second * cap + jnp.sum(jnp.where(lane_e == second, rank, 0.0), axis=1, keepdims=True).astype(jnp.int32)
    score = sc_ref[...]
    ex = jnp.exp(score - jnp.max(score, axis=-1, keepdims=True))
    route = grp_ref[...] * (ex / jnp.sum(ex, axis=-1, keepdims=True))
    rw_a, rw_b = route[:, 0:1], route[:, 1:2]
    lane_c = lax.broadcasted_iota(jnp.int32, (tokens, cap), 1)

    def pack(e):
        lane = lane_c + e * cap
        place = ((lane == slot_a) | (lane == slot_b)).astype(BF16)
        out[e] = dot(place, ffn[...], ((0,), (0,))).astype(BF16)

    def offset(i):
        return n // 2 + jnp.where(lax.rem(i, 2) == 0, i // 2, -((i + 1) // 2))

    def dispatch_copy(e):
        return pltpu.make_async_remote_copy(
            src_ref=out.at[e], dst_ref=recv.at[me], send_sem=d_ss.at[e], recv_sem=d_rs.at[me],
            device_id=(e, tp), device_id_type=MESH)

    def dispatch_arrival(s):
        return pltpu.make_async_remote_copy(
            src_ref=out.at[s], dst_ref=recv.at[s], send_sem=d_ss.at[s], recv_sem=d_rs.at[s],
            device_id=(s, tp), device_id_type=MESH)

    def answer_copy(s):
        return pltpu.make_async_remote_copy(
            src_ref=ans.at[s], dst_ref=back.at[me], send_sem=a_ss.at[s], recv_sem=a_rs.at[me],
            device_id=(s, tp), device_id_type=MESH)

    def answer_arrival(e):
        return pltpu.make_async_remote_copy(
            src_ref=ans.at[e], dst_ref=back.at[e], send_sem=a_ss.at[e], recv_sem=a_rs.at[e],
            device_id=(e, tp), device_id_type=MESH)

    for copy in pair_copies():
        copy.wait_send()
    def pair_arrival():
        return [
            pltpu.make_async_remote_copy(
                src_ref=cpair.at[1 - par], dst_ref=cpair.at[1 - par], send_sem=c1s, recv_sem=c1r,
                device_id=(partner, tp), device_id_type=MESH),
            pltpu.make_async_remote_copy(
                src_ref=spair.at[1 - par], dst_ref=spair.at[1 - par], send_sem=s1s, recv_sem=s1r,
                device_id=(partner, tp), device_id_type=MESH),
        ]

    for copy in pair_arrival():
        copy.wait_recv()

    def unpack(c, s):
        return (s[2:3], s[1:2], c.astype(F32), s[0:1])

    both = join(unpack(cpair[0], spair[0]), unpack(cpair[1], spair[1]))
    cgrp[grp] = both[2].astype(BF16)
    sgrp[grp] = stats(both[0], both[1], both[3])

    def group_copies(g):
        to = (g * 2 + par, tp)
        return [
            pltpu.make_async_remote_copy(
                src_ref=cgrp.at[grp], dst_ref=cgrp.at[grp], send_sem=c2s.at[g], recv_sem=c2r.at[grp],
                device_id=to, device_id_type=MESH),
            pltpu.make_async_remote_copy(
                src_ref=sgrp.at[grp], dst_ref=sgrp.at[grp], send_sem=s2s.at[g], recv_sem=s2r.at[grp],
                device_id=to, device_id_type=MESH),
        ]

    def group_arrivals(g):
        at = (g * 2 + par, tp)
        return [
            pltpu.make_async_remote_copy(
                src_ref=cgrp.at[g], dst_ref=cgrp.at[g], send_sem=c2s.at[g], recv_sem=c2r.at[g],
                device_id=at, device_id_type=MESH),
            pltpu.make_async_remote_copy(
                src_ref=sgrp.at[g], dst_ref=sgrp.at[g], send_sem=s2s.at[g], recv_sem=s2r.at[g],
                device_id=at, device_id_type=MESH),
        ]

    def send_group(g, c):
        for copy in group_copies(g):
            copy.start()
        return c

    lax.fori_loop(grp + 1, groups, send_group, 0)

    def send_tokens(i, c):
        e = lax.rem(me + offset(i), n)
        pack(e)
        dispatch_copy(e).start()
        return c

    lax.fori_loop(0, n - 1, send_tokens, 0)
    pack(me)
    for load in loads:
        load.wait()

    def expert(chosen):
        gate = dot(chosen, wg[...])
        up = dot(chosen, wu[...])
        hidden = (gate / (1.0 + jnp.exp(-gate)) * up).astype(BF16)
        return dot(hidden, wd[...]).astype(BF16)

    ans[me] = expert(out[me])

    ent[...] = jnp.zeros(ent.shape, F32)
    row1 = jnp.zeros((1, hd), F32)

    def enter(g, carry):
        total, peak, nor = carry
        for copy in group_arrivals(g):
            copy.wait_recv()
        total, peak, mem, nor = join((total, peak, ent[...], nor), unpack(cgrp[g], sgrp[g]))
        ent[...] = mem
        return total, peak, nor

    total, peak, nor = lax.fori_loop(0, grp, enter, (row1, row1 + FLOOR, row1))
    joined = join((total, peak, ent[...], nor), unpack(cpair[0], spair[0]))
    odd = par == 1
    m_in = jnp.where(odd, joined[1], peak)
    n_in = jnp.where(odd, joined[3], nor)
    c_in = jnp.where(odd, joined[2], ent[...])

    carried = b_col + m_in[:, 0:1]
    decay = jnp.where(cid <= rid, b_col - b_row + i_row, -jnp.inf)
    peaks = jnp.maximum(carried, jnp.max(decay, axis=-1, keepdims=True))
    across = jnp.exp(carried - peaks)
    scores = dot(q_ref[...], k_ref[...], ((1,), (1,))) * (hd**-0.5) * jnp.exp(decay - peaks)
    qf = q_ref[...].astype(F32)
    den = jnp.sum(scores, axis=-1, keepdims=True) + across * jnp.sum(qf * n_in, axis=-1, keepdims=True)
    num = dot(scores.astype(BF16), v_ref[...]) + across * dot(q_ref[...], c_in.astype(BF16))
    cell = num / jnp.maximum(jnp.abs(den), jnp.exp(-peaks))
    head[...] = (cell * hs_ref[...]).astype(BF16)

    def part_copy(j):
        return pltpu.make_async_remote_copy(
            src_ref=pout.at[j], dst_ref=prec.at[tp], send_sem=p_ss.at[j], recv_sem=p_rs.at[tp],
            device_id=(me, j), device_id_type=MESH)

    def part_arrival(j):
        return pltpu.make_async_remote_copy(
            src_ref=pout.at[j], dst_ref=prec.at[j], send_sem=p_ss.at[j], recv_sem=p_rs.at[j],
            device_id=(me, j), device_id_type=MESH)

    def project(j):
        pout[j] = dot(head[pl.ds(pl.multiple_of(j * rows, rows), rows), :], wo[...]).astype(BF16)

    def send_part(i, c):
        j = lax.rem(tp + i, nt)
        project(j)
        part_copy(j).start()
        return c

    lax.fori_loop(1, nt, send_part, 0)
    project(tp)

    def serve(i, c):
        s = lax.rem(me - offset(i) + n, n)
        dispatch_arrival(s).wait_recv()
        ans[s] = expert(recv[s])
        answer_copy(s).start()
        return c

    lax.fori_loop(0, n - 1, serve, 0)

    def mix(i, total):
        j = lax.rem(tp + i, nt)
        part_arrival(j).wait_recv()
        return total + prec[j].astype(F32)

    projected = pout[tp].astype(F32)
    for i in range(1, nt):
        projected = mix(i, projected)
    mixed_ref[...] = rms(projected, ps_ref[...]).astype(BF16)

    def weigh(e, block):
        lane = lane_c + e * cap
        w = jnp.where(lane == slot_a, rw_a, jnp.where(lane == slot_b, rw_b, 0.0))
        high = w.astype(BF16)
        low = (w - high.astype(F32)).astype(BF16)
        return dot(high, block) + dot(low, block)

    acc[...] = weigh(me, ans[me])

    def collect(i, c):
        e = lax.rem(me + offset(i), n)
        answer_arrival(e).wait_recv()
        acc[...] += weigh(e, back[e])
        return c

    lax.fori_loop(0, n - 1, collect, 0)
    routed_ref[...] = acc[...].astype(BF16)

    def finish(i, c):
        e = lax.rem(me + i, n)
        dispatch_copy(e).wait_send()
        answer_copy(e).wait_send()
        return c

    lax.fori_loop(1, n, finish, 0)

    def finish_group(g, c):
        for copy in group_copies(g):
            copy.wait_send()
        return c

    lax.fori_loop(grp + 1, groups, finish_group, 0)
    for i in range(1, nt):
        part_copy(lax.rem(tp + i, nt)).wait_send()


def relay_kernel(
    n, nt, cap,
    q_ref, k_ref, v_ref, ig_ref, fg_ref, fb_ref, hs_ref, wo_hbm, ps_ref,
    x_ref, es_ref, ids_ref, grp_ref, sc_ref, wg_hbm, wu_hbm, wd_hbm,
    mixed_ref, routed_ref,
    wg, wu, wd, wo, tok, info, xs, xr, ya, yb, own, part, ret, acc,
    cpair, spair, cgrp, sgrp, ent, head, pout, prec,
    wsem, t_ss, t_rs, i_ss, i_rs, x_ss, x_rs, y_ss, y_rs, r_ss, r_rs, c1s, c1r, s1s, s1r, c2s, c2r, s2s, s2r, p_ss, p_rs,
):
    me = lax.axis_index("ep")
    tp = lax.axis_index("tp")
    groups = n // 2
    grp = me // 2
    par = lax.rem(me, 2)
    partner = me + 1 - 2 * par
    tokens, width = x_ref.shape
    length, hd = q_ref.shape
    rows = mixed_ref.shape[0]

    barrier = pltpu.get_barrier_semaphore()

    def greet(i, c):
        pl.semaphore_signal(barrier, inc=1, device_id=(lax.rem(me + i, n), tp), device_id_type=MESH)
        return c

    lax.fori_loop(1, n, greet, 0)
    for j in range(1, nt):
        pl.semaphore_signal(barrier, inc=1, device_id=(me, lax.rem(tp + j, nt)), device_id_type=MESH)

    loads = [
        pltpu.make_async_copy(wg_hbm.at[0], wg, wsem.at[0]),
        pltpu.make_async_copy(wu_hbm.at[0], wu, wsem.at[1]),
        pltpu.make_async_copy(wd_hbm.at[0], wd, wsem.at[2]),
        pltpu.make_async_copy(wo_hbm.at[pl.ds(pl.multiple_of(tp * hd, hd), hd)], wo, wsem.at[3]),
    ]
    for load in loads:
        load.start()

    tok[grp] = rms(x_ref[...].astype(F32), es_ref[...]).astype(BF16)
    half = tokens // 2

    def tok_copy(s, h, to, sem):
        rows_of = pl.ds(h * half, half)
        return pltpu.make_async_remote_copy(
            src_ref=tok.at[s, rows_of], dst_ref=tok.at[s, rows_of], send_sem=t_ss.at[sem, h],
            recv_sem=t_rs.at[s, h], device_id=(to * 2 + par, tp), device_id_type=MESH)

    def info_copy(g, s):
        return pltpu.make_async_remote_copy(
            src_ref=info.at[s], dst_ref=info.at[s], send_sem=i_ss.at[g],
            recv_sem=i_rs.at[s], device_id=(g * 2 + par, tp), device_id_type=MESH)

    def swap_copy(kind, s):
        src, dst, ss, rs = ((xs, xr, x_ss, x_rs), (ya, yb, y_ss, y_rs))[kind]
        return pltpu.make_async_remote_copy(
            src_ref=src.at[s], dst_ref=dst.at[s], send_sem=ss.at[s],
            recv_sem=rs.at[s], device_id=(partner, tp), device_id_type=MESH)

    def ret_copy(s, slot, to):
        return pltpu.make_async_remote_copy(
            src_ref=part.at[s], dst_ref=ret.at[slot], send_sem=r_ss.at[s],
            recv_sem=r_rs.at[slot], device_id=(to * 2 + par, tp), device_id_type=MESH)


    pl.semaphore_wait(barrier, n - 1 + nt - 1)
    for h in range(2):
        @pl.when(grp + 1 < groups)
        def _():
            tok_copy(grp, h, grp + 1, grp).start()

        @pl.when(grp > 0)
        def _():
            tok_copy(grp, h, grp - 1, groups).start()

    ids = ids_ref[...]
    first, second = ids[:, 0:1], ids[:, 1:2]
    lane_e = lax.broadcasted_iota(jnp.int32, (tokens, n), 1)
    named = ((lane_e == first) | (lane_e == second)).astype(F32)
    tr = lax.broadcasted_iota(jnp.int32, (tokens, tokens), 0)
    tc = lax.broadcasted_iota(jnp.int32, (tokens, tokens), 1)
    rank = dot((tc < tr).astype(BF16), named.astype(BF16))
    slot_a = first * cap + jnp.sum(jnp.where(lane_e == first, rank, 0.0), axis=1, keepdims=True).astype(jnp.int32)
    slot_b = second * cap + jnp.sum(jnp.where(lane_e == second, rank, 0.0), axis=1, keepdims=True).astype(jnp.int32)
    score = sc_ref[...]
    ex = jnp.exp(score - jnp.max(score, axis=-1, keepdims=True))
    route = grp_ref[...] * (ex / jnp.sum(ex, axis=-1, keepdims=True))
    rw_a, rw_b = route[:, 0:1], route[:, 1:2]
    lane_c = lax.broadcasted_iota(jnp.int32, (tokens, cap), 1)

    lane_i = lax.broadcasted_iota(jnp.int32, (tokens, 128), 1)
    table = jnp.where(lane_i == 0, slot_a.astype(F32), jnp.where(lane_i == 1, slot_b.astype(F32),
        jnp.where(lane_i == 2, rw_a, jnp.where(lane_i == 3, rw_b, 0.0))))
    wide = info.shape[2]
    table = jnp.concatenate([table, jnp.zeros((wide - tokens, 128), F32)], axis=0)
    info[grp] = table.T[0:8]

    def send_info(j, c):
        info_copy(lax.rem(grp + j, groups), grp).start()
        return c

    lax.fori_loop(1, groups, send_info, 0)

    def columns(s):
        wide_cols = jnp.concatenate([info[s], jnp.zeros((120, info.shape[2]), F32)], axis=0).T[0:tokens]
        return (wide_cols[:, 0:1].astype(jnp.int32), wide_cols[:, 1:2].astype(jnp.int32),
                wide_cols[:, 2:3], wide_cols[:, 3:4])

    def place(cols_s, e):
        lane = lane_c + e * cap
        return ((lane == cols_s[0]) | (lane == cols_s[1])).astype(BF16)

    def pack(s):
        xs[s] = dot(place(columns(s), partner), tok[s], ((0,), (0,))).astype(BF16)
        swap_copy(0, s).start()

    pack(grp)

    fg = fg_ref[...]
    lk = jnp.minimum(fg, 0.0) - jnp.log1p(jnp.exp(-jnp.abs(fg))) + fb_ref[...]
    rid = lax.broadcasted_iota(jnp.int32, (length, length), 0)
    cid = lax.broadcasted_iota(jnp.int32, (length, length), 1)
    upper = (rid <= cid).astype(F32)
    b_row = dot(jnp.broadcast_to(lk, (8, length)), upper, precision=lax.Precision.HIGHEST)[0:1]
    i_row = ig_ref[...]
    last = b_row[:, length - 1 : length]
    g_row = last - b_row + i_row
    m_loc = jnp.max(g_row, axis=-1, keepdims=True)
    which = lax.broadcasted_iota(jnp.int32, (128, length), 0)
    cols = jnp.where(which == 0, b_row, g_row).T
    b_col = cols[:, 0:1]
    g_col = cols[:, 1:2]
    kw = k_ref[...].astype(F32) * (jnp.exp(g_col - m_loc) * (hd**-0.5))
    c_loc = dot(kw.astype(BF16), v_ref[...], ((0,), (0,)))
    n_loc = jnp.sum(kw, axis=0, keepdims=True)
    stat_id = lax.broadcasted_iota(jnp.int32, (8, hd), 0)

    def stats(total, peak, nor):
        return jnp.where(stat_id == 0, nor, jnp.where(stat_id == 1, peak, total))

    cpair[par] = c_loc.astype(BF16)
    spair[par] = stats(last, m_loc, n_loc)

    def pair_copies():
        return [
            pltpu.make_async_remote_copy(
                src_ref=cpair.at[par], dst_ref=cpair.at[par], send_sem=c1s, recv_sem=c1r,
                device_id=(partner, tp), device_id_type=MESH),
            pltpu.make_async_remote_copy(
                src_ref=spair.at[par], dst_ref=spair.at[par], send_sem=s1s, recv_sem=s1r,
                device_id=(partner, tp), device_id_type=MESH),
        ]

    for copy in pair_copies():
        copy.start()

    for copy in pair_copies():
        copy.wait_send()
    def pair_arrival():
        return [
            pltpu.make_async_remote_copy(
                src_ref=cpair.at[1 - par], dst_ref=cpair.at[1 - par], send_sem=c1s, recv_sem=c1r,
                device_id=(partner, tp), device_id_type=MESH),
            pltpu.make_async_remote_copy(
                src_ref=spair.at[1 - par], dst_ref=spair.at[1 - par], send_sem=s1s, recv_sem=s1r,
                device_id=(partner, tp), device_id_type=MESH),
        ]

    for copy in pair_arrival():
        copy.wait_recv()

    def unpack(c, s):
        return (s[2:3], s[1:2], c.astype(F32), s[0:1])

    both = join(unpack(cpair[0], spair[0]), unpack(cpair[1], spair[1]))
    cgrp[grp] = both[2].astype(BF16)
    sgrp[grp] = stats(both[0], both[1], both[3])

    def group_copies(g):
        to = (g * 2 + par, tp)
        return [
            pltpu.make_async_remote_copy(
                src_ref=cgrp.at[grp], dst_ref=cgrp.at[grp], send_sem=c2s.at[g], recv_sem=c2r.at[grp],
                device_id=to, device_id_type=MESH),
            pltpu.make_async_remote_copy(
                src_ref=sgrp.at[grp], dst_ref=sgrp.at[grp], send_sem=s2s.at[g], recv_sem=s2r.at[grp],
                device_id=to, device_id_type=MESH),
        ]

    def group_arrivals(g):
        at = (g * 2 + par, tp)
        return [
            pltpu.make_async_remote_copy(
                src_ref=cgrp.at[g], dst_ref=cgrp.at[g], send_sem=c2s.at[g], recv_sem=c2r.at[g],
                device_id=at, device_id_type=MESH),
            pltpu.make_async_remote_copy(
                src_ref=sgrp.at[g], dst_ref=sgrp.at[g], send_sem=s2s.at[g], recv_sem=s2r.at[g],
                device_id=at, device_id_type=MESH),
        ]

    def send_group(g, c):
        for copy in group_copies(g):
            copy.start()
        return c

    lax.fori_loop(grp + 1, groups, send_group, 0)

    for load in loads:
        load.wait()

    def weigh(cols_s, e, block):
        lane = lane_c + e * cap
        w = jnp.where(lane == cols_s[0], cols_s[2], jnp.where(lane == cols_s[1], cols_s[3], 0.0))
        high = w.astype(BF16)
        low = (w - high.astype(F32)).astype(BF16)
        return dot(high, block) + dot(low, block)

    def experts(s):
        cols_s = columns(s)
        mine = dot(place(cols_s, me), tok[s], ((0,), (0,))).astype(BF16)
        swap_copy(0, s).wait_recv()
        chosen = jnp.concatenate([xr[s], mine], axis=0)
        gate = dot(chosen, wg[...])
        up = dot(chosen, wu[...])
        hidden = (gate / (1.0 + jnp.exp(-gate)) * up).astype(BF16)
        answer = dot(hidden, wd[...]).astype(BF16)
        ya[s] = answer[0:cap]
        swap_copy(1, s).start()
        own[s] = answer[cap:]

    def combined(s):
        cols_s = columns(s)
        swap_copy(1, s).wait_recv()
        return weigh(cols_s, me, own[s]) + weigh(cols_s, partner, yb[s])

    def hop(s):
        below = s < grp
        to = jnp.where(below, grp - 1, grp + 1)
        slot = jnp.where(to == s, jnp.where(below, s, groups), s)
        return ret_copy(s, slot, to)

    def where_is(i):
        d, side = 1 + i // 2, lax.rem(i, 2)
        s = grp + d * (2 * side - 1)
        return s, (s >= 0) & (s < groups)

    def at_end(s):
        return jnp.where(s < grp, grp == groups - 1, grp == 0)

    def take(i, c):
        s, valid = where_is(i)

        @pl.when(valid)
        def _():
            onward = jnp.where(s < grp, grp + 1, grp - 1)
            for h in range(2):
                tok_copy(s, h, grp, s).wait_recv()

                @pl.when(jnp.logical_not(at_end(s)))
                def _():
                    tok_copy(s, h, onward, s).start()

            info_copy(s, s).wait_recv()
            pack(s)

        return c

    def work(i, c):
        s, valid = where_is(i)

        @pl.when(valid)
        def _():
            experts(s)

        return c

    def close(i, c):
        s, valid = where_is(i)

        @pl.when(valid & at_end(s))
        def _():
            part[s] = combined(s).astype(BF16)
            hop(s).start()

        return c

    def serve(d, c):
        for step in (take, work, close):
            lax.fori_loop(2 * d, 2 * d + 2, step, 0)
        return c

    experts(grp)
    lax.fori_loop(0, 1, serve, 0)

    ent[...] = jnp.zeros(ent.shape, F32)
    row1 = jnp.zeros((1, hd), F32)

    def enter(g, carry):
        total, peak, nor = carry
        for copy in group_arrivals(g):
            copy.wait_recv()
        total, peak, mem, nor = join((total, peak, ent[...], nor), unpack(cgrp[g], sgrp[g]))
        ent[...] = mem
        return total, peak, nor

    total, peak, nor = lax.fori_loop(0, grp, enter, (row1, row1 + FLOOR, row1))
    joined = join((total, peak, ent[...], nor), unpack(cpair[0], spair[0]))
    odd = par == 1
    m_in = jnp.where(odd, joined[1], peak)
    n_in = jnp.where(odd, joined[3], nor)
    c_in = jnp.where(odd, joined[2], ent[...])

    carried = b_col + m_in[:, 0:1]
    decay = jnp.where(cid <= rid, b_col - b_row + i_row, -jnp.inf)
    peaks = jnp.maximum(carried, jnp.max(decay, axis=-1, keepdims=True))
    across = jnp.exp(carried - peaks)
    scores = dot(q_ref[...], k_ref[...], ((1,), (1,))) * (hd**-0.5) * jnp.exp(decay - peaks)
    qf = q_ref[...].astype(F32)
    den = jnp.sum(scores, axis=-1, keepdims=True) + across * jnp.sum(qf * n_in, axis=-1, keepdims=True)
    num = dot(scores.astype(BF16), v_ref[...]) + across * dot(q_ref[...], c_in.astype(BF16))
    cell = num / jnp.maximum(jnp.abs(den), jnp.exp(-peaks))
    head[...] = (cell * hs_ref[...]).astype(BF16)

    def part_copy(j):
        return pltpu.make_async_remote_copy(
            src_ref=pout.at[j], dst_ref=prec.at[tp], send_sem=p_ss.at[j], recv_sem=p_rs.at[tp],
            device_id=(me, j), device_id_type=MESH)

    def part_arrival(j):
        return pltpu.make_async_remote_copy(
            src_ref=pout.at[j], dst_ref=prec.at[j], send_sem=p_ss.at[j], recv_sem=p_rs.at[j],
            device_id=(me, j), device_id_type=MESH)

    def project(j):
        pout[j] = dot(head[pl.ds(pl.multiple_of(j * rows, rows), rows), :], wo[...]).astype(BF16)

    def send_part(i, c):
        j = lax.rem(tp + i, nt)
        project(j)
        part_copy(j).start()
        return c

    lax.fori_loop(1, nt, send_part, 0)
    project(tp)

    lax.fori_loop(1, groups - 1, serve, 0)

    def give_back(j, c):
        s, valid = where_is(2 * (groups - 1) - 1 - j)

        @pl.when(valid & jnp.logical_not(at_end(s)))
        def _():
            mine = combined(s)
            ret_copy(s, s, grp).wait_recv()
            part[s] = (mine + ret[s].astype(F32)).astype(BF16)
            hop(s).start()

        return c

    lax.fori_loop(0, 2 * (groups - 1), give_back, 0)

    def mix(i, total):
        j = lax.rem(tp + i, nt)
        part_arrival(j).wait_recv()
        return total + prec[j].astype(F32)

    projected = pout[tp].astype(F32)
    for i in range(1, nt):
        projected = mix(i, projected)
    mixed_ref[...] = rms(projected, ps_ref[...]).astype(BF16)

    acc[...] = combined(grp)
    for slot, there in ((grp, grp + 1 < groups), (groups, grp > 0)):
        @pl.when(there)
        def _():
            ret_copy(grp, slot, grp).wait_recv()
            acc[...] += ret[slot].astype(F32)

    routed_ref[...] = acc[...].astype(BF16)

    def finish(s, c):
        swap_copy(0, s).wait_send()
        swap_copy(1, s).wait_send()

        @pl.when(s != grp)
        def _():
            hop(s).wait_send()
            info_copy(s, grp).wait_send()

        for h in range(2):
            @pl.when((s != grp) & jnp.logical_not(at_end(s)))
            def _():
                tok_copy(s, h, grp, s).wait_send()

        return c

    lax.fori_loop(0, groups, finish, 0)
    for h in range(2):
        @pl.when(grp + 1 < groups)
        def _():
            tok_copy(grp, h, grp, grp).wait_send()

        @pl.when(grp > 0)
        def _():
            tok_copy(grp, h, grp, groups).wait_send()

    def finish_group(g, c):
        for copy in group_copies(g):
            copy.wait_send()
        return c

    lax.fori_loop(grp + 1, groups, finish_group, 0)
    for i in range(1, nt):
        part_copy(lax.rem(tp + i, nt)).wait_send()


def shards(
    n, nt,
    memory_query_matrix, memory_key_matrix, memory_value_matrix,
    input_gate_logits, forget_gate_logits, forget_log_boosts,
    head_norm_scale, memory_output_matrix, projection_norm_scale,
    second_batch_rows, expert_prenorm_scale, selected_expert_index,
    group_route_probability, expert_choice_scores,
    expert_gate_matrix, expert_up_matrix, expert_down_matrix,
):
    length, hd = memory_query_matrix.shape
    tokens, width = second_batch_rows.shape
    hidden = expert_gate_matrix.shape[2]
    cap = 2 * selected_expert_index.shape[1] * tokens // n
    cap = -(-cap // 16) * 16
    rows = length // nt
    vm = pl.BlockSpec(memory_space=pltpu.VMEM)
    hbm = pl.BlockSpec(memory_space=pl.ANY)
    dma = pltpu.SemaphoreType.DMA
    slots = pltpu.VMEM((n, cap, width), BF16)
    groups = n // 2
    relay = groups * tokens * width * 6 < 24 * 1024 * 1024
    wide = -(-tokens // 128) * 128
    some = pltpu.VMEM((groups, cap, width), BF16)
    if relay:
        body = relay_kernel
        buffers = [
            pltpu.VMEM((groups, tokens, width), BF16),
            pltpu.VMEM((groups, 8, wide), F32),
            some, some, some, some, some,
            pltpu.VMEM((groups, tokens, width), BF16),
            pltpu.VMEM((groups + 1, tokens, width), BF16),
            pltpu.VMEM((tokens, width), F32),
        ]
        sems = [dma((groups + 1, 2)), dma((groups, 2))] + [dma((groups,))] * 7 + [dma((groups + 1,))]
    else:
        body = kernel
        buffers = [
            slots, slots, slots, slots,
            pltpu.VMEM((tokens, width), BF16),
            pltpu.VMEM((tokens, width), F32),
        ]
        sems = [dma((n,))] * 4
    return pl.pallas_call(
        functools.partial(body, n, nt, cap),
        out_shape=(
            jax.ShapeDtypeStruct((rows, width), BF16),
            jax.ShapeDtypeStruct((tokens, width), BF16),
        ),
        in_specs=[vm] * 7 + [hbm] + [vm] * 6 + [hbm] * 3,
        out_specs=(vm, vm),
        scratch_shapes=[
            pltpu.VMEM((width, hidden), BF16),
            pltpu.VMEM((width, hidden), BF16),
            pltpu.VMEM((hidden, width), BF16),
            pltpu.VMEM((hd, width), BF16),
            *buffers,
            pltpu.VMEM((2, hd, hd), BF16),
            pltpu.VMEM((2, 8, hd), F32),
            pltpu.VMEM((n // 2, hd, hd), BF16),
            pltpu.VMEM((n // 2, 8, hd), F32),
            pltpu.VMEM((hd, hd), F32),
            pltpu.VMEM((length, hd), BF16),
            pltpu.VMEM((nt, rows, width), BF16),
            pltpu.VMEM((nt, rows, width), BF16),
            dma((4,)),
            *sems,
            dma, dma, dma, dma,
            dma((n // 2,)), dma((n // 2,)), dma((n // 2,)), dma((n // 2,)),
            dma((nt,)), dma((nt,)),
        ],
        compiler_params=pltpu.CompilerParams(
            collective_id=0, has_side_effects=True, vmem_limit_bytes=62 * 1024 * 1024
        ),
    )(
        memory_query_matrix, memory_key_matrix, memory_value_matrix,
        input_gate_logits, forget_gate_logits, forget_log_boosts,
        head_norm_scale[None], memory_output_matrix, projection_norm_scale[None],
        second_batch_rows, expert_prenorm_scale[None], selected_expert_index,
        group_route_probability[:, None], expert_choice_scores,
        expert_gate_matrix, expert_up_matrix, expert_down_matrix,
    )


def solution(mesh):
    return jax.shard_map(
        functools.partial(shards, mesh.shape["ep"], mesh.shape["tp"]),
        mesh=mesh,
        in_specs=(
            P("ep", "tp"), P("ep", "tp"), P("ep", "tp"),
            P("tp", "ep"), P("tp", "ep"), P("tp", "ep"),
            P("tp"), P(), P(),
            P(("ep", "tp"), None), P(), P(("ep", "tp"), None),
            P(("ep", "tp")), P(("ep", "tp"), None),
            P("ep", None, None), P("ep", None, None), P("ep", None, None),
        ),
        out_specs=(P(("ep", "tp"), None), P(("ep", "tp"), None)),
        check_vma=False,
    )
```
